32 devices in a mesh: fs: 8 (over z, x), tp: 4 (over y, core).
Axes of the slice: x: 2, y: 2, z: 4, core: 2. Of those that a mesh axis runs over, the one named last changes fastest.
Arguments:
- inputs: bfloat16 [2048, 2048], P('fs'), may hold values from -6 to 6
- cotangent: bfloat16 [2048, 2048], P('fs'), may hold values from -8 to 8
- up_weight: float32 [2048, 2944], P('fs', 'tp'), may hold values from -0.125 to 0.125
- gate_weight: float32 [2048, 2944], P('fs', 'tp'), may hold values from -0.125 to 0.125
- down_weight: float32 [2944, 2048], P('tp', 'fs'), may hold values from -0.109375 to 0.109375
- up_scale: float32 [2944], P('tp'), may hold values from 0.5 to 2
- gate_scale: float32 [2944], P('tp'), may hold values from 0.5 to 2
- down_scale: float32 [2048], replicated, may hold values from 0.5 to 2
- conv_weight: float32 [3, 2944], P(None, 'tp'), may hold values from -3.5 to 3.5
- conv_bias: float32 [2944], P('tp'), may hold values from -3 to 3
Outputs:
- grad_input: bfloat16 [2048, 2048], P('fs')
- grad_up: float32 [2048, 2944], P('fs', 'tp')
- grad_gate: float32 [2048, 2944], P('fs', 'tp')
- grad_down: float32 [2944, 2048], P('tp', 'fs')
- grad_conv: float32 [3, 2944], P(None, 'tp')
- grad_bias: float32 [2944], P('tp')
The draws below stay inside these ranges and needn't reach their ends.
All inputs are finite; a program needn't handle non-finite values.
Results may differ from the reference program's by a relative error of at most 0.018.
Values may be sent and summed in bfloat16 or wider, within the bound.
No kernel may reach another device: no remote copies, remote signals or barrier semaphores. Data moves between devices by JAX's collectives and lax.ppermute only.
A program may use at most 64 MiB of HBM per device.

```python
import math
import jax
import jax.numpy as jnp
from jax import lax

D = 2048
FF = 2944
TAPS = 3
TOK_DEV = 256
TOKENS = 2048
N_TP = 4


def raised(values, key, source, target, blocks, factor):
    def block_of(position):
        return (jnp.arange(values.shape[position]) // (values.shape[position] // blocks)).reshape((-1,) + (1,) * (values.ndim - 1 - position))

    near = jax.random.permutation(key, blocks)[block_of(target)]
    second = (block_of(target) + blocks // 2) % blocks
    return jnp.where((block_of(source) == near) | (block_of(source) == second), factor * values, values)


def steps_of(stream_key, shape, pieces, low, top_value):
    level, own = 1.0, jax.random.fold_in(stream_key, 6)
    for position, blocks in pieces:
        draws = jnp.exp(jax.random.uniform(jax.random.fold_in(own, position), (blocks,), jnp.float32, low / len(pieces), top_value / len(pieces)))
        level = level * jnp.repeat(draws, shape[position] // blocks).reshape([-1 if axis == position else 1 for axis in range(len(shape))])
    return level


def gaussian(rng, dims, scale, bound, shards=(), dtype=jnp.bfloat16):
    loudness = steps_of(rng, dims, shards, -0.22, 0.18) if shards else 1.0
    values = jax.random.normal(rng, dims, jnp.float32) * scale * loudness
    return jnp.minimum(jnp.maximum(values, -bound), bound).astype(dtype)


def gaussian_with(stream_key, extent, spread, bound, split, heavy, kind=jnp.bfloat16):
    values = spread * jax.random.normal(stream_key, extent, jnp.float32)
    if split:
        values = values * steps_of(stream_key, extent, split, -0.22, 0.18)
    return jnp.clip(raised(values, jax.random.fold_in(stream_key, 3), *heavy), -bound, bound).astype(kind)


def setup_inputs(seed: int = 0) -> dict:
    splits = jax.random.split(jax.random.key(seed), 11)
    return {
        "inputs": gaussian(splits[0], (TOKENS, D), 1.0, 6.0, ((0, 8),)),
        "cotangent": gaussian_with(splits[1], (TOKENS, D), 1.0, 8.0, ((0, 8),), (0, 1, 8, 2.0)),
        "up_weight": gaussian(splits[2], (D, FF), D ** -0.5, 0.125, ((0, 8), (1, 4)), jnp.float32),
        "gate_weight": gaussian(splits[3], (D, FF), D ** -0.5, 0.125, ((0, 8), (1, 4)), jnp.float32),
        "down_weight": gaussian(splits[4], (FF, D), FF ** -0.5, 0.109375, ((0, 4), (1, 8)), jnp.float32),
        "up_scale": jnp.clip(jnp.exp(math.log(2.0) - 1.3862944 * jax.random.uniform(splits[5], (FF,), jnp.float32) ** steps_of(splits[5], (FF,), ((0, 4),), -0.2, 0.2)), 0.5, 2.0),
        "gate_scale": jnp.clip(jnp.exp(math.log(2.0) - 1.3862944 * jax.random.uniform(splits[6], (FF,), jnp.float32) ** steps_of(splits[6], (FF,), ((0, 4),), -0.2, 0.2)), 0.5, 2.0),
        "down_scale": jnp.clip(jnp.exp(jax.random.uniform(splits[7], (D,), jnp.float32, math.log(0.5), math.log(2.0))), 0.5, 2.0),
        "conv_weight": gaussian(splits[8], (TAPS, FF), TAPS ** -0.5, 3.5, ((1, 4),), jnp.float32),
        "conv_bias": gaussian(splits[9], (FF,), 0.5, 3.0, ((0, 4),), jnp.float32),
    }


def causal_conv(act, conv_weight, conv_bias):
    seq_view = act.reshape(-1, TOK_DEV, act.shape[-1])
    padded = jnp.pad(seq_view, ((0, 0), (TAPS - 1, 0), (0, 0)))
    result = conv_bias + jnp.zeros_like(seq_view)
    for offset in range(TAPS):
        result = result + padded[:, offset:offset + TOK_DEV] * conv_weight[offset]
    return (result.reshape(act.shape), padded)

def conv_back(conv_cot, padded, conv_weight):
    seq_cot = conv_cot.reshape(-1, TOK_DEV, conv_cot.shape[-1])
    padded_cot = jnp.pad(seq_cot, ((0, 0), (0, TAPS - 1), (0, 0)))
    act_cot = jnp.zeros_like(seq_cot)
    tap_grads = []
    for offset in range(TAPS):
        shift_start = TAPS - 1 - offset
        act_cot = act_cot + conv_weight[offset] * padded_cot[:, shift_start:shift_start + TOK_DEV]
        tap_grads.append(lax.optimization_barrier(jnp.sum(seq_cot * padded[:, offset:offset + TOK_DEV], axis=(0, 1))))
    return (act_cot.reshape(conv_cot.shape), jnp.stack(tap_grads), lax.optimization_barrier(jnp.sum(seq_cot, axis=(0, 1))))

def reference(inputs, cotangent, up_weight, gate_weight, down_weight, up_scale, gate_scale, down_scale, conv_weight, conv_bias):
    up_half = up_weight.astype(jnp.bfloat16)
    gate_half = gate_weight.astype(jnp.bfloat16)
    down_half = down_weight.astype(jnp.bfloat16)
    up_act = jnp.dot(inputs, up_half, preferred_element_type=jnp.float32) * up_scale
    gate_act = jnp.dot(inputs, gate_half, preferred_element_type=jnp.float32) * gate_scale
    conv_out, padded = causal_conv(up_act, conv_weight, conv_bias)
    gelu_val, gelu_back = jax.vjp(jax.nn.gelu, conv_out)
    hidden = (gelu_val * gate_act).astype(jnp.bfloat16)
    scaled_cot = (cotangent.astype(jnp.float32) * down_scale).astype(jnp.bfloat16)
    hidden_cot = lax.dot_general(scaled_cot, down_half, (((1,), (1,)), ((), ())), preferred_element_type=jnp.float32)
    gate_cot = (hidden_cot * gelu_val * gate_scale).astype(jnp.bfloat16)
    conv_cot, = gelu_back(hidden_cot * gate_act)
    act_cot, grad_conv, grad_bias = conv_back(conv_cot, padded, conv_weight)
    up_cot = (act_cot * up_scale).astype(jnp.bfloat16)
    width = FF // N_TP
    total = jnp.zeros(inputs.shape, jnp.float32)
    for block_index in range(N_TP):
        start = block_index * width
        part = lax.dot_general(up_cot[:, start:start + width], up_half[:, start:start + width], (((1,), (1,)), ((), ())), preferred_element_type=jnp.float32)
        part = part + lax.dot_general(gate_cot[:, start:start + width], gate_half[:, start:start + width], (((1,), (1,)), ((), ())), preferred_element_type=jnp.float32)
        total = total + lax.optimization_barrier(part.astype(jnp.bfloat16)).astype(jnp.float32)
    grad_input = total.astype(jnp.bfloat16)
    grad_up = lax.dot_general(inputs, up_cot, (((0,), (0,)), ((), ())), preferred_element_type=jnp.float32)
    grad_gate = lax.dot_general(inputs, gate_cot, (((0,), (0,)), ((), ())), preferred_element_type=jnp.float32)
    grad_down = lax.dot_general(hidden, scaled_cot, (((0,), (0,)), ((), ())), preferred_element_type=jnp.float32)
    return (grad_input, grad_up, grad_gate, grad_down, grad_conv, grad_bias)
```

```python
import jax
import jax.numpy as jnp
from jax import lax
from jax.sharding import Mesh
from jax.sharding import PartitionSpec as P

TAPS = 3


def dot_f32(left, right, left_dim, right_dim):
    return lax.dot_general(
        left, right, (((left_dim,), (right_dim,)), ((), ())), preferred_element_type=jnp.float32
    )


def swap(value):
    return lax.ppermute(value, "fx", [(0, 1), (1, 0)])


def column(vector):
    return vector[:, None]


def later(act, step, position):
    if step == 0:
        return act
    moved = jnp.pad(act, ((0, 0), (step, 0)))[:, : act.shape[1]]
    return jnp.where(position >= step, moved, 0.0)


def earlier(act, step, position, length):
    if step == 0:
        return act
    moved = jnp.pad(act, ((0, 0), (0, step)))[:, step:]
    return jnp.where(position < length - step, moved, 0.0)


def sum_over_fz(value, n_fz):
    if n_fz & (n_fz - 1):
        return lax.psum(value, "fz")
    step = 1
    while step < n_fz:
        value = value + lax.ppermute(value, "fz", [(i, i ^ step) for i in range(n_fz)])
        step *= 2
    return value


def sum_over_tp(partial, n_tp):
    rows = partial.shape[0] // n_tp
    me = lax.axis_index("tp")

    def piece(index):
        return lax.dynamic_slice_in_dim(partial, index * rows, rows, 0)

    total = piece(me).astype(jnp.float32)
    for shift in range(1, n_tp):
        ring = [(i, (i + shift) % n_tp) for i in range(n_tp)]
        got = lax.ppermute(piece((me + shift) % n_tp), "tp", ring)
        total = total + got.astype(jnp.float32)
    own = total.astype(jnp.bfloat16)
    result = lax.dynamic_update_slice_in_dim(jnp.zeros_like(partial), own, me * rows, 0)
    for shift in range(1, n_tp):
        ring = [(i, (i + shift) % n_tp) for i in range(n_tp)]
        got = lax.ppermute(own, "tp", ring)
        source = (me - shift) % n_tp
        result = lax.dynamic_update_slice_in_dim(result, got, source * rows, 0)
    return result


def make_on_device(n_fz, n_tp):
    def on_device(
        inputs,
        cotangent,
        up_weight,
        gate_weight,
        down_weight,
        up_scale,
        gate_scale,
        down_scale,
        conv_weight,
        conv_bias,
    ):
        bf16 = jnp.bfloat16
        low = lax.axis_index("fx") == 0
        length = inputs.shape[0]
        half = down_weight.shape[0] // 2
        width = down_weight.shape[1]

        def mine(value, axis=0):
            first, second = jnp.split(value, 2, axis=axis)
            return jnp.where(low, first, second)

        def theirs(value, axis=0):
            first, second = jnp.split(value, 2, axis=axis)
            return jnp.where(low, second, first)

        def in_order(own, other, axis):
            return jnp.concatenate(
                [jnp.where(low, own, other), jnp.where(low, other, own)], axis=axis
            )

        def gather(weights):
            stored = jnp.stack([w.astype(bf16) for w in weights])
            block = in_order(mine(stored, 1), swap(theirs(stored, 1)), 2)
            return lax.all_gather(block, "fz", axis=2, tiled=True)

        full_pair = gather([up_weight.T, gate_weight.T])
        full_down = gather([down_weight])[0]
        tokens = jnp.concatenate([inputs, swap(inputs)], axis=0)
        scaled_own = (cotangent.astype(jnp.float32) * down_scale).astype(bf16)
        scaled_cot = jnp.concatenate([scaled_own, swap(scaled_own)], axis=0)
        up_col = column(mine(up_scale))
        gate_col = column(mine(gate_scale))
        taps = mine(conv_weight, 1)
        bias_col = column(mine(conv_bias))
        position = lax.broadcasted_iota(jnp.int32, (1, 2 * length), 1) % length

        up_act = dot_f32(full_pair[0], tokens, 1, 1) * up_col
        gate_act = dot_f32(full_pair[1], tokens, 1, 1) * gate_col
        shifted = [later(up_act, TAPS - 1 - k, position) for k in range(TAPS)]
        conv_out = bias_col
        for k in range(TAPS):
            conv_out = conv_out + shifted[k] * column(taps[k])
        gelu_val, gelu_back = jax.vjp(jax.nn.gelu, conv_out)
        hidden = (gelu_val * gate_act).astype(bf16)

        def scatter(term):
            return lax.psum_scatter(term.astype(bf16), "fz", scatter_dimension=1, tiled=True)

        def finish(block):
            return in_order(mine(block, 1), swap(theirs(block, 1)), 0).astype(jnp.float32)

        grad_down = finish(scatter(dot_f32(hidden, scaled_cot, 1, 0)))
        hidden_cot = dot_f32(full_down, scaled_cot, 1, 1)
        gate_cot = (hidden_cot * gelu_val * gate_col).astype(bf16)
        grad_gate = finish(scatter(dot_f32(gate_cot, tokens, 1, 0))).T
        (conv_cot,) = gelu_back(hidden_cot * gate_act)
        act_cot = jnp.zeros_like(conv_cot)
        for k in range(TAPS):
            act_cot = act_cot + column(taps[k]) * earlier(conv_cot, TAPS - 1 - k, position, length)
        up_cot = (act_cot * up_col).astype(bf16)
        grad_up = finish(scatter(dot_f32(up_cot, tokens, 1, 0))).T

        def input_part(start):
            up_side = dot_f32(up_cot[:, start : start + length], full_pair[0], 0, 0)
            return up_side + dot_f32(gate_cot[:, start : start + length], full_pair[1], 0, 0)

        other_part = swap(input_part(length).astype(bf16))
        partial = (input_part(0) + other_part.astype(jnp.float32)).astype(bf16)
        grad_input = sum_over_tp(partial, n_tp)

        sums = [jnp.sum(conv_cot * shifted[k], axis=1) for k in range(TAPS)]
        sums = jnp.stack(sums + [jnp.sum(conv_cot, axis=1)])
        sums = sum_over_fz(sums, n_fz)
        sums = in_order(sums, swap(sums), 1)
        return (grad_input, grad_up, grad_gate, grad_down, sums[:TAPS], sums[TAPS])

    return on_device


def solution(mesh):
    n_fs, n_tp = mesh.shape["fs"], mesh.shape["tp"]
    split = Mesh(mesh.devices.reshape(n_fs // 2, 2, n_tp), ("fz", "fx", "tp"))
    fs = ("fz", "fx")
    in_specs = (
        P(fs, None),
        P(fs, None),
        P(fs, "tp"),
        P(fs, "tp"),
        P("tp", fs),
        P("tp"),
        P("tp"),
        P(),
        P(None, "tp"),
        P("tp"),
    )
    out_specs = (P(fs, None), P(fs, "tp"), P(fs, "tp"), P("tp", fs), P(None, "tp"), P("tp"))
    return jax.shard_map(
        make_on_device(n_fs // 2, n_tp),
        mesh=split,
        in_specs=in_specs,
        out_specs=out_specs,
        check_vma=False,
    )
```

```python
import jax
import jax.numpy as jnp
from jax import lax
from jax.sharding import Mesh
from jax.sharding import PartitionSpec as P

TAPS = 3


def dot_f32(left, right, left_dim, right_dim):
    return lax.dot_general(
        left, right, (((left_dim,), (right_dim,)), ((), ())), preferred_element_type=jnp.float32
    )


def swap(value):
    return lax.ppermute(value, "fx", [(0, 1), (1, 0)])


def column(vector):
    return vector[:, None]


def later(act, step, position):
    if step == 0:
        return act
    moved = jnp.pad(act, ((0, 0), (step, 0)))[:, : act.shape[1]]
    return jnp.where(position >= step, moved, 0.0)


def earlier(act, step, position, length):
    if step == 0:
        return act
    moved = jnp.pad(act, ((0, 0), (0, step)))[:, step:]
    return jnp.where(position < length - step, moved, 0.0)


def sum_over_fz(value, n_fz):
    if n_fz & (n_fz - 1):
        return lax.psum(value, "fz")
    step = 1
    while step < n_fz:
        value = value + lax.ppermute(value, "fz", [(i, i ^ step) for i in range(n_fz)])
        step *= 2
    return value


def sum_over_tp(partial, n_tp):
    rows = partial.shape[0] // n_tp
    me = lax.axis_index("tp")

    def piece(index):
        return lax.dynamic_slice_in_dim(partial, index * rows, rows, 0)

    total = piece(me).astype(jnp.float32)
    for shift in range(1, n_tp):
        ring = [(i, (i + shift) % n_tp) for i in range(n_tp)]
        got = lax.ppermute(piece((me + shift) % n_tp), "tp", ring)
        total = total + got.astype(jnp.float32)
    own = total.astype(jnp.bfloat16)
    result = lax.dynamic_update_slice_in_dim(jnp.zeros_like(partial), own, me * rows, 0)
    for shift in range(1, n_tp):
        ring = [(i, (i + shift) % n_tp) for i in range(n_tp)]
        got = lax.ppermute(own, "tp", ring)
        source = (me - shift) % n_tp
        result = lax.dynamic_update_slice_in_dim(result, got, source * rows, 0)
    return result


def make_on_device(n_fz, n_tp):
    def on_device(
        inputs,
        cotangent,
        up_weight,
        gate_weight,
        down_weight,
        up_scale,
        gate_scale,
        down_scale,
        conv_weight,
        conv_bias,
    ):
        bf16 = jnp.bfloat16
        low = lax.axis_index("fx") == 0
        length = inputs.shape[0]
        width = down_weight.shape[1]

        def mine(value, axis=0):
            first, second = jnp.split(value, 2, axis=axis)
            return jnp.where(low, first, second)

        def theirs(value, axis=0):
            first, second = jnp.split(value, 2, axis=axis)
            return jnp.where(low, second, first)

        def in_order(own, other, axis):
            return jnp.concatenate(
                [jnp.where(low, own, other), jnp.where(low, other, own)], axis=axis
            )

        def gather(block):
            return lax.all_gather(block, "fz", axis=block.ndim - 1, tiled=True)

        pair = jnp.stack([up_weight.T.astype(bf16), gate_weight.T.astype(bf16)])
        own_pair = gather(mine(pair, 1))
        other_pair = gather(swap(theirs(pair, 1)))
        stored_down = down_weight.astype(bf16)
        full_down = gather(in_order(mine(stored_down), swap(theirs(stored_down)), 1))
        first_pair = jnp.where(low, own_pair, other_pair)
        second_pair = jnp.where(low, other_pair, own_pair)
        full_pair = jnp.concatenate(
            [
                block[:, :, i * width : (i + 1) * width]
                for i in range(n_fz)
                for block in (first_pair, second_pair)
            ],
            axis=2,
        )
        tokens = jnp.concatenate([inputs, swap(inputs)], axis=0)
        even_rows = [tokens[:, 2 * i * width : (2 * i + 1) * width] for i in range(n_fz)]
        odd_rows = [tokens[:, (2 * i + 1) * width : (2 * i + 2) * width] for i in range(n_fz)]
        even_rows = jnp.concatenate(even_rows, axis=1)
        odd_rows = jnp.concatenate(odd_rows, axis=1)
        own_rows = jnp.where(low, even_rows, odd_rows)
        other_rows = jnp.where(low, odd_rows, even_rows)
        scaled_own = (cotangent.astype(jnp.float32) * down_scale).astype(bf16)
        scaled_cot = jnp.concatenate([scaled_own, swap(scaled_own)], axis=0)
        up_col = column(mine(up_scale))
        gate_col = column(mine(gate_scale))
        taps = mine(conv_weight, 1)
        bias_col = column(mine(conv_bias))
        position = lax.broadcasted_iota(jnp.int32, (1, 2 * length), 1) % length

        up_act = dot_f32(full_pair[0], tokens, 1, 1) * up_col
        gate_act = dot_f32(full_pair[1], tokens, 1, 1) * gate_col
        shifted = [later(up_act, TAPS - 1 - k, position) for k in range(TAPS)]
        conv_out = bias_col
        for k in range(TAPS):
            conv_out = conv_out + shifted[k] * column(taps[k])
        gelu_val, gelu_back = jax.vjp(jax.nn.gelu, conv_out)
        hidden = (gelu_val * gate_act).astype(bf16)

        def scatter(term):
            return lax.psum_scatter(term.astype(bf16), "fz", scatter_dimension=1, tiled=True)

        def finish(block):
            return in_order(mine(block, 1), swap(theirs(block, 1)), 0).astype(jnp.float32)

        hidden = lax.optimization_barrier(hidden)
        down_term = dot_f32(hidden, scaled_cot, 1, 0).astype(bf16)
        down_term, scaled_cot = lax.optimization_barrier((down_term, scaled_cot))
        grad_down = finish(scatter(down_term))
        hidden_cot = dot_f32(full_down, scaled_cot, 1, 1)
        gate_cot = (hidden_cot * gelu_val * gate_col).astype(bf16)
        (conv_cot,) = gelu_back(hidden_cot * gate_act)
        act_cot = jnp.zeros_like(conv_cot)
        for k in range(TAPS):
            act_cot = act_cot + column(taps[k]) * earlier(conv_cot, TAPS - 1 - k, position, length)
        up_cot = (act_cot * up_col).astype(bf16)
        cots = jnp.concatenate([gate_cot, up_cot], axis=0)
        sent = scatter(dot_f32(cots, other_rows, 1, 0))
        kept = scatter(dot_f32(cots, own_rows, 1, 0))
        received = swap(sent)
        half = up_cot.shape[0]
        grad_gate = in_order(kept[:half], received[:half], 0).astype(jnp.float32).T
        grad_up = in_order(kept[half:], received[half:], 0).astype(jnp.float32).T

        def input_part(start):
            up_side = dot_f32(up_cot[:, start : start + length], full_pair[0], 0, 0)
            return up_side + dot_f32(gate_cot[:, start : start + length], full_pair[1], 0, 0)

        other_part = swap(input_part(length).astype(bf16))
        partial = (input_part(0) + other_part.astype(jnp.float32)).astype(bf16)
        grad_input = sum_over_tp(partial, n_tp)

        sums = [jnp.sum(conv_cot * shifted[k], axis=1) for k in range(TAPS)]
        sums = jnp.stack(sums + [jnp.sum(conv_cot, axis=1)])
        sums = sum_over_fz(sums, n_fz)
        sums = in_order(sums, swap(sums), 1)
        return (grad_input, grad_up, grad_gate, grad_down, sums[:TAPS], sums[TAPS])

    return on_device


def solution(mesh):
    n_fs, n_tp = mesh.shape["fs"], mesh.shape["tp"]
    split = Mesh(mesh.devices.reshape(n_fs // 2, 2, n_tp), ("fz", "fx", "tp"))
    fs = ("fz", "fx")
    in_specs = (
        P(fs, None),
        P(fs, None),
        P(fs, "tp"),
        P(fs, "tp"),
        P("tp", fs),
        P("tp"),
        P("tp"),
        P(),
        P(None, "tp"),
        P("tp"),
    )
    out_specs = (P(fs, None), P(fs, "tp"), P(fs, "tp"), P("tp", fs), P(None, "tp"), P("tp"))
    return jax.shard_map(
        make_on_device(n_fs // 2, n_tp),
        mesh=split,
        in_specs=in_specs,
        out_specs=out_specs,
        check_vma=False,
    )
```
